32 devices in a mesh: fs: 8 (over z, x), tp: 4 (over y, core).
Axes of the slice: x: 2, y: 2, z: 4, core: 2. Of those that a mesh axis runs over, the one named last changes fastest.
Arguments:
- saved_input: bfloat16 [49152, 2048], P(('fs', 'tp')), may hold values from -6 to 6
- value_cotangent: bfloat16 [49152, 1024], P(('fs', 'tp')), may hold values from -0.0546875 to 0.0546875
- decay_cotangent: bfloat16 [49152, 16], P(('fs', 'tp')), may hold values from -0.02734375 to 0.02734375
- value_master: float32 [2048, 1024], P('fs', 'tp'), may hold values from -6 to 6
- value_factor: bfloat16 [2048, 256], P('fs'), may hold values from -0.22097087 to 0.22097087
- value_mean: float32 [256, 1024], P('fs', 'tp'), may hold values from -0.625 to 0.625
- value_second: float32 [256, 1024], P('fs', 'tp'), may hold values from 0.0001 to 0.1
- decay_master: float32 [2048, 16], replicated, may hold values from -6 to 6
- decay_mean: float32 [2048, 16], replicated, may hold values from -0.625 to 0.625
- decay_second: float32 [2048, 16], replicated, may hold values from 0.001 to 0.01
Outputs:
- value_step: float32 [2048, 1024], P('fs', 'tp')
- value_new: float32 [2048, 1024], P('fs', 'tp')
- value_copy: bfloat16 [2048, 1024], P(None, 'tp')
- mean_new: float32 [256, 1024], P('fs', 'tp')
- second_new: float32 [256, 1024], P('fs', 'tp')
- decay_step: float32 [2048, 16], replicated
- decay_copy: bfloat16 [2048, 16], replicated
The draws below stay inside these ranges and needn't reach their ends.
All inputs are finite; a program needn't handle non-finite values.
Results may differ from the reference program's by a relative error of at most 0.0004.
Values may be sent and summed in bfloat16 or wider, within the bound.
No kernel may reach another device: no remote copies, remote signals or barrier semaphores. Data moves between devices by JAX's collectives and lax.ppermute only.
A program may use at most 64 MiB of HBM per device.

```python
import math
import jax
import jax.numpy as jnp
from jax import lax

D = 2048
HG = 16
GW = 1024
RANK = 256
TOKENS = 49152


def draw_value_factor(key, part):
    base_key, tilt_key = jax.random.split(jax.random.fold_in(key, 17))
    base = jnp.clip(jax.random.normal(base_key, (D, RANK), jnp.float32), -4.0, 4.0)
    place = jnp.arange(D, dtype=jnp.float32)[:, None] / D
    jitter = jax.random.uniform(tilt_key, (D, 1), jnp.float32)
    scale = 10.0 ** (0.5 * place + 0.5 * jitter) * 0.25 * D ** (-0.5)
    return (base * scale).astype(jnp.bfloat16)


def draw_value_second(key, part):
    entry_key, tilt_key = jax.random.split(jax.random.fold_in(key, 29))
    place = jnp.arange(GW, dtype=jnp.float32)[None, :] / GW
    jitter = jax.random.uniform(tilt_key, (1, GW), jnp.float32)
    column = 100.0 ** (0.5 * place + 0.5 * jitter)
    entry = 10.0 ** jax.random.uniform(entry_key, (RANK, GW), jnp.float32)
    return (0.0001 * entry * column).astype(jnp.float32)


def strengthened(result, own_key, source, target, parts, factor):
    owner, partner = [(jnp.arange(result.shape[axis_at]) // (result.shape[axis_at] // parts)).reshape([-1 if axis == axis_at else 1 for axis in range(result.ndim)]) for axis_at in (source, target)]
    chosen = jax.random.permutation(own_key, parts)[partner]
    strong = (owner == chosen) | (owner == (partner + parts // 2) % parts)
    return jnp.where(strong, factor * result, result)


def shard_levels(stream_key, extent, cuts, smallest, largest):
    def one(position, blocks):
        steps = jax.random.uniform(jax.random.fold_in(jax.random.fold_in(stream_key, 6), position), (blocks,), jnp.float32, smallest / len(cuts), largest / len(cuts))
        return jnp.repeat(jnp.exp(steps), extent[position] // blocks).reshape((-1,) + (1,) * (len(extent) - position - 1))

    level = one(*cuts[0])
    for cut in cuts[1:]:
        level = level * one(*cut)
    return level


def centred(stream_key, dims, spread, reach, pieces=(), kind=jnp.bfloat16):
    drawn = spread * jax.random.normal(stream_key, dims, jnp.float32)
    if pieces:
        drawn = drawn * shard_levels(stream_key, dims, pieces, -0.22, 0.18)
    return jnp.clip(drawn, -reach, reach).astype(kind)


def bell_draw_with(own_key, extent, deviation, bound, shards, heavy, kind=jnp.bfloat16):
    drawn = deviation * jax.random.normal(own_key, extent, jnp.float32)
    if shards:
        drawn = drawn * shard_levels(own_key, extent, shards, -0.22, 0.18)
    return jnp.clip(strengthened(drawn, jax.random.fold_in(own_key, 3), *heavy), -bound, bound).astype(kind)


def setup_inputs(seed: int = 0) -> dict:
    key_list = jax.random.split(jax.random.key(seed), 11)
    return {
        "saved_input": centred(key_list[0], (TOKENS, D), 1.0, 6.0, ((0, 32),)),
        "value_cotangent": bell_draw_with(key_list[1], (TOKENS, GW), (TOKENS ** -0.5), 0.0546875, ((0, 32),), (0, 1, 32, 2.75)),
        "decay_cotangent": centred(key_list[2], (TOKENS, HG), (TOKENS ** -0.5), 0.02734375, ((0, 32),)),
        "value_master": centred(key_list[3], (D, GW), 1.0, 6.0, ((0, 8), (1, 4)), jnp.float32),
        "value_factor": draw_value_factor(jax.random.fold_in(key_list[10], 71), 0),
        "value_mean": centred(key_list[5], (RANK, GW), 0.1, 0.625, ((0, 8), (1, 4)), jnp.float32),
        "value_second": draw_value_second(jax.random.fold_in(key_list[10], 71), 0),
        "decay_master": centred(key_list[7], (D, HG), 1.0, 6.0, (), jnp.float32),
        "decay_mean": centred(key_list[8], (D, HG), 0.1, 0.625, (), jnp.float32),
        "decay_second": jnp.clip(jnp.exp(jax.random.uniform(key_list[9], (D, HG), jnp.float32, math.log(0.001), math.log(0.01))), 0.001, 0.01),
    }


BETA_ONE = 0.9
BETA_TWO = 0.99
ADAM_EPS = 1e-08
RMS_EPS = 1e-06
LEARN_RATE = 0.05
TOKEN_DIMS = (((0,), (0,)), ((), ()))

def adam_direction(moment_one, moment_two, gradient):
    mean_new = BETA_ONE * moment_one + (1.0 - BETA_ONE) * gradient
    second_new = BETA_TWO * moment_two + (1.0 - BETA_TWO) * gradient * gradient
    return (mean_new, second_new, mean_new / (jnp.sqrt(second_new) + ADAM_EPS))

def reference(saved_input, value_cotangent, decay_cotangent, value_master, value_factor, value_mean, value_second, decay_master, decay_mean, decay_second):
    value_grad = lax.dot_general(saved_input, value_cotangent, TOKEN_DIMS, preferred_element_type=jnp.float32)
    factor_wide = value_factor.astype(jnp.float32)
    projected = lax.dot_general(factor_wide, value_grad, TOKEN_DIMS, precision=lax.Precision.HIGHEST, preferred_element_type=jnp.float32)
    mean_new, second_new, direction = adam_direction(value_mean, value_second, projected)
    raw_update = jnp.dot(factor_wide, direction, precision=lax.Precision.HIGHEST, preferred_element_type=jnp.float32)
    value_step = raw_update * lax.rsqrt(jnp.mean(raw_update * raw_update) + RMS_EPS)
    value_new = value_master - LEARN_RATE * value_step
    value_copy = value_new.astype(jnp.bfloat16)
    decay_grad = lax.dot_general(saved_input, decay_cotangent, TOKEN_DIMS, preferred_element_type=jnp.float32)
    unused_mean, unused_second, decay_step = adam_direction(decay_mean, decay_second, decay_grad)
    decay_copy = (decay_master - LEARN_RATE * decay_step).astype(jnp.bfloat16)
    return (value_step, value_new, value_copy, mean_new, second_new, decay_step, decay_copy)
```

```python
import jax
import jax.numpy as jnp
from jax import lax
from jax.sharding import PartitionSpec as P

BETA_ONE = 0.9
BETA_TWO = 0.99
ADAM_EPS = 1e-08
RMS_EPS = 1e-06
LEARN_RATE = 0.05
TOKEN_DIMS = (((0,), (0,)), ((), ()))
F32 = jnp.float32
BF16 = jnp.bfloat16


def adam_direction(moment_one, moment_two, gradient):
    mean_new = BETA_ONE * moment_one + (1.0 - BETA_ONE) * gradient
    second_new = BETA_TWO * moment_two + (1.0 - BETA_TWO) * gradient * gradient
    return (mean_new, second_new, mean_new / (jnp.sqrt(second_new) + ADAM_EPS))


def split_two(wide):
    high = lax.optimization_barrier(wide.astype(BF16))
    low = (wide - high.astype(F32)).astype(BF16)
    return high, low


def swap(block, axis, bit):
    count = lax.axis_size(axis)
    return lax.ppermute(block, axis, [(i, i ^ bit) for i in range(count)])


def direct_gather(block, axis):
    count = lax.axis_size(axis)
    me = lax.axis_index(axis)
    parts = [block] + [
        lax.ppermute(block, axis, [(i, (i + step) % count) for i in range(count)])
        for step in range(1, count)
    ]
    out = jnp.zeros((count,) + block.shape, block.dtype)
    for step, part in enumerate(parts):
        out = lax.dynamic_update_index_in_dim(out, part, (me - step) % count, 0)
    return out


def xor_bits(count):
    bits, bit = [], 1
    while bit < count:
        bits.append(bit)
        bit *= 2
    assert bit == count
    return bits


def xor_reduce_scatter(pieces, axis):
    left = list(range(len(pieces)))
    for bit in xor_bits(len(pieces)):
        sent = [o for o in left if o & bit]
        left = [o for o in left if not o & bit]
        for o in sent:
            pieces[o ^ bit] = pieces[o ^ bit] + swap(pieces[o], axis, bit)
    return pieces[0]


def xor_gather(block, axis):
    found = [block]
    for bit in xor_bits(lax.axis_size(axis)):
        found = found + [swap(part, axis, bit) for part in found]
    return found


def local(
    saved_input,
    value_cotangent,
    decay_cotangent,
    value_master,
    value_factor,
    value_mean,
    value_second,
    decay_master,
    decay_mean,
    decay_second,
):
    fs_count, tp_count = lax.axis_size("fs"), lax.axis_size("tp")
    tp_me, fs_me = lax.axis_index("tp"), lax.axis_index("fs")
    width_in, rank = saved_input.shape[1], value_factor.shape[1]
    columns = value_cotangent.shape[1] // tp_count
    heads = decay_cotangent.shape[1]
    shard_rows = value_factor.shape[0]
    half_rows = shard_rows // 2
    core = tp_me % 2

    half = lax.dynamic_slice_in_dim(value_factor, core * half_rows, half_rows, 0)
    mine = direct_gather(half, "fs")
    other = swap(mine, "tp", 1)
    first = jnp.where(core == 0, mine, other)
    second = jnp.where(core == 0, other, mine)
    factor = jnp.stack([first, second], 1).reshape(width_in, rank)

    gradient = lax.dot_general(
        saved_input, value_cotangent, TOKEN_DIMS, preferred_element_type=F32
    )
    high, low = split_two(gradient)
    decay_local = lax.dot_general(
        decay_cotangent, saved_input, TOKEN_DIMS, preferred_element_type=F32
    )

    decay_width = width_in // tp_count
    pieces = []
    for offset in range(tp_count):
        member = tp_me ^ offset
        term = jnp.zeros((rank, columns), F32)
        for part in (high, low):
            block = lax.dynamic_slice_in_dim(part, member * columns, columns, 1)
            term = term + lax.dot_general(factor, block, TOKEN_DIMS, preferred_element_type=F32)
        decay_block = lax.dynamic_slice_in_dim(decay_local, member * decay_width, decay_width, 1)
        pieces.append(
            jnp.concatenate(
                [
                    term.reshape(fs_count, rank // fs_count, columns),
                    decay_block.reshape(fs_count, -1, columns),
                ],
                1,
            )
        )
    block_sum = xor_reduce_scatter(pieces, "tp")
    owned = jnp.sum(lax.all_to_all(block_sum, "fs", 0, 0, tiled=True), 0)
    rank_rows = rank // fs_count
    projected, decay_part = owned[:rank_rows], owned[rank_rows:]
    mean_new, second_new, direction = adam_direction(value_mean, value_second, projected)

    spread = direct_gather(jnp.concatenate([direction, decay_part], 0), "fs")
    direction_all = spread[:, :rank_rows].reshape(rank, columns)
    decay_block = spread[:, rank_rows:].reshape(heads, decay_width)

    parts = split_two(direction_all)
    raw_all = jnp.dot(factor, parts[0], preferred_element_type=F32) + jnp.dot(
        factor, parts[1], preferred_element_type=F32
    )
    squares = jnp.broadcast_to(jnp.sum(raw_all * raw_all), (8, 128))
    for bit in xor_bits(tp_count):
        squares = squares + swap(squares, "tp", bit)
    entries = width_in * value_cotangent.shape[1]
    scale = lax.rsqrt(squares[0, 0] / entries + RMS_EPS)
    raw_update = lax.dynamic_slice_in_dim(raw_all, fs_me * shard_rows, shard_rows, 0)
    value_step = raw_update * scale
    value_new = value_master - LEARN_RATE * value_step
    value_copy = direct_gather(value_new.astype(BF16), "fs").reshape(width_in, columns)

    decay_grad = jnp.zeros((heads, width_in), F32)
    for offset, part in enumerate(xor_gather(decay_block, "tp")):
        decay_grad = lax.dynamic_update_slice_in_dim(
            decay_grad, part, (tp_me ^ offset) * decay_width, 1
        )
    unused_mean, unused_second, decay_step = adam_direction(
        decay_mean, decay_second, decay_grad.T
    )
    decay_copy = (decay_master - LEARN_RATE * decay_step).astype(BF16)
    return (value_step, value_new, value_copy, mean_new, second_new, decay_step, decay_copy)


def solution(mesh):
    in_specs = (
        P(("fs", "tp"), None),
        P(("fs", "tp"), None),
        P(("fs", "tp"), None),
        P("fs", "tp"),
        P("fs", None),
        P("fs", "tp"),
        P("fs", "tp"),
        P(),
        P(),
        P(),
    )
    out_specs = (
        P("fs", "tp"),
        P("fs", "tp"),
        P(None, "tp"),
        P("fs", "tp"),
        P("fs", "tp"),
        P(),
        P(),
    )
    return jax.shard_map(local, mesh=mesh, in_specs=in_specs, out_specs=out_specs, check_vma=False)
```

```python
import jax
import jax.numpy as jnp
from jax import lax
from jax.experimental import pallas as pl
from jax.experimental.pallas import tpu as pltpu
from jax.sharding import PartitionSpec as P

BETA_ONE = 0.9
BETA_TWO = 0.99
ADAM_EPS = 1e-08
RMS_EPS = 1e-06
LEARN_RATE = 0.05
VMEM_BYTES = 24 * 1024 * 1024
TOKEN_DIMS = (((0,), (0,)), ((), ()))
F32 = jnp.float32
BF16 = jnp.bfloat16


def adam_direction(moment_one, moment_two, gradient):
    mean_new = BETA_ONE * moment_one + (1.0 - BETA_ONE) * gradient
    second_new = BETA_TWO * moment_two + (1.0 - BETA_TWO) * gradient * gradient
    return (mean_new, second_new, mean_new / (jnp.sqrt(second_new) + ADAM_EPS))


def split_two(wide):
    high = lax.reduce_precision(wide, 8, 7)
    return high.astype(BF16), (wide - high).astype(BF16)


def swap(block, axis, bit):
    count = lax.axis_size(axis)
    return lax.ppermute(block, axis, [(i, i ^ bit) for i in range(count)])


def xor_bits(count):
    bits, bit = [], 1
    while bit < count:
        bits.append(bit)
        bit *= 2
    assert bit == count
    return bits


def xor_reduce_scatter(pieces, axis):
    left = list(range(len(pieces)))
    for bit in xor_bits(len(pieces)):
        sent = [o for o in left if o & bit]
        left = [o for o in left if not o & bit]
        for o in sent:
            pieces[o ^ bit] = pieces[o ^ bit] + swap(pieces[o], axis, bit)
    return pieces[0]


def xor_gather(block, axis):
    found = [block]
    for bit in xor_bits(lax.axis_size(axis)):
        found = found + [swap(part, axis, bit) for part in found]
    return found


def pair_gather(block, axis):
    pair = jnp.stack([block, swap(block, axis, 1)])
    return [pair] + [swap(pair, axis, o) for o in range(2, lax.axis_size(axis), 2)]


def whole(shape):
    return pl.BlockSpec(memory_space=pltpu.VMEM)


def run(kernel, indices, operands, shapes, name):
    return pl.pallas_call(
        kernel,
        in_specs=[pl.BlockSpec(memory_space=pltpu.SMEM)] + [whole(x.shape) for x in operands],
        out_specs=[whole(x.shape) for x in shapes],
        out_shape=shapes,
        compiler_params=pltpu.CompilerParams(vmem_limit_bytes=VMEM_BYTES),
        name=name,
    )(indices, *operands)


def assemble_factor(parts, others, indices):
    count = 2 * len(parts)
    half_rows, rank = parts[0].shape[1:]

    def kernel(index, *refs):
        out = refs[-1]
        for k in range(len(parts)):
            for side in range(2):
                member = index[0] ^ (2 * k + side)
                base = member * (2 * half_rows)
                mine = pl.multiple_of(base + index[1] * half_rows, half_rows)
                other = pl.multiple_of(base + (1 - index[1]) * half_rows, half_rows)
                out[pl.ds(mine, half_rows), :] = refs[k][side]
                out[pl.ds(other, half_rows), :] = refs[len(parts) + k][side]

    shape = jax.ShapeDtypeStruct((count * 2 * half_rows, rank), BF16)
    return run(kernel, indices, parts + others, [shape], "assemble")[0]


def update_kernel(parts, factor, rank_rows, indices):
    count = 2 * len(parts)
    total, columns = parts[0].shape[1:]
    rows = factor.shape[0]

    def kernel(index, *refs):
        pieces, matrix, raw, squares, decay, gathered = refs[:-5], *refs[-5:]
        for k in range(len(parts)):
            for side in range(2):
                member = index[0] ^ (2 * k + side)
                start = pl.multiple_of(member * rank_rows, rank_rows)
                gathered[pl.ds(start, rank_rows), :] = pieces[k][side, :rank_rows]
                decay[member] = pieces[k][side, rank_rows:]
        wide = gathered[...]
        high = wide.astype(BF16)
        low = (wide - high.astype(F32)).astype(BF16)
        block = rows // 4
        acc = jnp.zeros((8, columns), F32)
        for at in range(4):
            left = matrix[at * block : (at + 1) * block, :]
            value = jnp.dot(left, high, preferred_element_type=F32) + jnp.dot(
                left, low, preferred_element_type=F32
            )
            raw[at * block : (at + 1) * block, :] = value
            acc = acc + jnp.sum((value * value).reshape(block // 8, 8, columns), 0)
        squares[...] = jnp.full((8, 128), jnp.sum(acc), F32)

    return pl.pallas_call(
        kernel,
        in_specs=[pl.BlockSpec(memory_space=pltpu.SMEM)]
        + [whole(x.shape) for x in parts]
        + [whole(factor.shape)],
        out_specs=[
            whole((rows, columns)),
            whole((8, 128)),
            whole((count, total - rank_rows, columns)),
        ],
        out_shape=[
            jax.ShapeDtypeStruct((rows, columns), F32),
            jax.ShapeDtypeStruct((8, 128), F32),
            jax.ShapeDtypeStruct((count, total - rank_rows, columns), F32),
        ],
        scratch_shapes=[pltpu.VMEM((count * rank_rows, columns), F32)],
        compiler_params=pltpu.CompilerParams(vmem_limit_bytes=VMEM_BYTES),
        name="update",
    )(indices, *parts, factor)


def finish(raw, terms, masters, offsets, entries, indices):
    rows, columns = raw.shape
    shard = masters[0].shape[-2]

    def kernel(index, raw_ref, *refs):
        squares = refs[0][...]
        for ref in refs[1 : len(terms)]:
            squares = squares + ref[...]
        scale = lax.rsqrt(squares * (1.0 / entries) + RMS_EPS)[0:1, 0:1]
        step_ref, new_ref, copy_ref = refs[-3:]
        at = len(terms)
        for ref, members in zip(refs[at:-3], offsets):
            for side, offset in enumerate(members):
                start = pl.multiple_of((index[0] ^ offset) * shard, shard)
                step = raw_ref[pl.ds(start, shard), :] * scale
                new = ref[side] - LEARN_RATE * step
                copy_ref[pl.ds(start, shard), :] = new.astype(BF16)
                if offset == 0:
                    step_ref[...] = step
                    new_ref[...] = new

    shapes = [
        jax.ShapeDtypeStruct((shard, columns), F32),
        jax.ShapeDtypeStruct((shard, columns), F32),
        jax.ShapeDtypeStruct((rows, columns), BF16),
    ]
    return run(kernel, indices, [raw] + terms + masters, shapes, "finish")


def local(
    saved_input,
    value_cotangent,
    decay_cotangent,
    value_master,
    value_factor,
    value_mean,
    value_second,
    decay_master,
    decay_mean,
    decay_second,
):
    fs_count, tp_count = lax.axis_size("fs"), lax.axis_size("tp")
    tp_me, fs_me = lax.axis_index("tp"), lax.axis_index("fs")
    width_in, rank = saved_input.shape[1], value_factor.shape[1]
    columns = value_cotangent.shape[1] // tp_count
    heads = decay_cotangent.shape[1]
    shard_rows = value_factor.shape[0]
    half_rows = shard_rows // 2
    core = tp_me & 1
    indices = jnp.stack([fs_me, core]).astype(jnp.int32)

    half = lax.dynamic_slice_in_dim(value_factor, core * half_rows, half_rows, 0)
    pair = jnp.stack([half, swap(half, "fs", 1)])
    pair, saved_input = lax.optimization_barrier((pair, saved_input))
    mine = [pair] + [swap(pair, "fs", o) for o in range(2, fs_count, 2)]

    high, low = split_two(
        lax.dot_general(saved_input, value_cotangent, TOKEN_DIMS, preferred_element_type=F32)
    )
    decay_local = lax.dot_general(
        decay_cotangent, saved_input, TOKEN_DIMS, preferred_element_type=F32
    )
    decay_width = width_in // tp_count
    decay_terms = [
        lax.dynamic_slice_in_dim(
            decay_local, (tp_me ^ offset) * decay_width, decay_width, 1
        ).reshape(fs_count, -1, columns)
        for offset in range(tp_count)
    ]
    late, decay_terms, high, low = lax.optimization_barrier((mine[1:], decay_terms, high, low))
    mine = [pair] + list(late)
    factor = assemble_factor(mine, [swap(part, "tp", 1) for part in mine], indices)
    early, factor = lax.optimization_barrier((value_master[None], factor))

    pieces = []
    for offset in range(tp_count):
        member = tp_me ^ offset
        term = jnp.zeros((rank, columns), F32)
        for part in (high, low):
            block = lax.dynamic_slice_in_dim(part, member * columns, columns, 1)
            term = term + lax.dot_general(factor, block, TOKEN_DIMS, preferred_element_type=F32)
        pieces.append(
            jnp.concatenate(
                [
                    term.reshape(fs_count, rank // fs_count, columns),
                    decay_terms[offset],
                ],
                1,
            )
        )
    masters = {0: early}
    bits = xor_bits(fs_count)
    for bit in bits:
        masters[bit] = swap(early, "fs", bit)
    block_sum = xor_reduce_scatter(pieces, "tp")
    top = bits[-1]
    masters[top], block_sum = lax.optimization_barrier((masters[top], block_sum))
    for bit in reversed(bits):
        for offset in sorted(masters):
            if offset ^ bit not in masters and not offset & bit and offset & -offset > bit:
                masters[offset ^ bit] = swap(masters[offset], "fs", bit)
    owned = jnp.sum(lax.all_to_all(block_sum, "fs", 0, 0, tiled=True), 0)
    rank_rows = rank // fs_count
    projected, decay_part = owned[:rank_rows], owned[rank_rows:]
    mean_new, second_new, direction = adam_direction(value_mean, value_second, projected)

    spread = pair_gather(jnp.concatenate([direction, decay_part], 0), "fs")
    raw_all, squares, decay_block = update_kernel(spread, factor, rank_rows, indices)
    for bit in xor_bits(tp_count)[:-1]:
        squares = squares + swap(squares, "tp", bit)
    terms = [squares] + [swap(squares, "tp", bit) for bit in xor_bits(tp_count)[-1:]]
    entries = width_in * value_cotangent.shape[1]
    value_step, value_new, value_copy = finish(
        raw_all,
        terms,
        [masters[offset] for offset in sorted(masters)],
        [(offset,) for offset in sorted(masters)],
        entries,
        indices,
    )

    decay_block = decay_block.reshape(heads, decay_width)
    decay_grad = jnp.zeros((heads, width_in), F32)
    for offset, part in enumerate(xor_gather(decay_block, "tp")):
        decay_grad = lax.dynamic_update_slice_in_dim(
            decay_grad, part, (tp_me ^ offset) * decay_width, 1
        )
    unused_mean, unused_second, decay_step = adam_direction(
        decay_mean, decay_second, decay_grad.T
    )
    decay_copy = (decay_master - LEARN_RATE * decay_step).astype(BF16)
    return (value_step, value_new, value_copy, mean_new, second_new, decay_step, decay_copy)


def solution(mesh):
    in_specs = (
        P(("fs", "tp"), None),
        P(("fs", "tp"), None),
        P(("fs", "tp"), None),
        P("fs", "tp"),
        P("fs", None),
        P("fs", "tp"),
        P("fs", "tp"),
        P(),
        P(),
        P(),
    )
    out_specs = (
        P("fs", "tp"),
        P("fs", "tp"),
        P(None, "tp"),
        P("fs", "tp"),
        P("fs", "tp"),
        P(),
        P(),
    )
    return jax.shard_map(local, mesh=mesh, in_specs=in_specs, out_specs=out_specs, check_vma=False)
```
